32 devices in a mesh: fs: 8 (over z, x), tp: 4 (over y, core).
Axes of the slice: x: 2, y: 2, z: 4, core: 2. Of those that a mesh axis runs over, the one named last changes fastest.
Arguments:
- normed_input: bfloat16 [8192, 2048], P('fs'), may hold values from -64 to 64
- query_cotangent: bfloat16 [8192, 1024], P('fs', 'tp'), may hold values from -6 to 6
- key_cotangent: bfloat16 [8192, 512], P('fs', 'tp'), may hold values from -6 to 6
- query_weight: float32 [2048, 1024], P('fs', 'tp'), may hold values from -6 to 6
- key_weight: float32 [2048, 512], P('fs', 'tp'), may hold values from -6 to 6
- query_basis: bfloat16 [1024, 128], P('tp'), may hold values from -1 to 1
- key_basis: bfloat16 [512, 128], P('tp'), may hold values from -1 to 1
- moment_mean: float32 [2, 2048, 128], P(None, 'fs'), may hold values from -3 to 3
- moment_square: float32 [2, 2048, 128], P(None, 'fs'), may hold values from 0.25 to 4
Outputs:
- query_step: float32 [2048, 1024], P('fs', 'tp')
- key_step: float32 [2048, 512], P('fs', 'tp')
- query_updated: float32 [2048, 1024], P('fs', 'tp')
- key_updated: float32 [2048, 512], P('fs', 'tp')
- query_copy: bfloat16 [2048, 1024], P('fs', 'tp')
- key_copy: bfloat16 [2048, 512], P('fs', 'tp')
- mean_updated: float32 [2, 2048, 128], P(None, 'fs')
- square_updated: float32 [2, 2048, 128], P(None, 'fs')
The draws below stay inside these ranges and needn't reach their ends.
All inputs are finite; a program needn't handle non-finite values.
Results may differ from the reference program's by a relative error of at most 0.0011.
Values sent between devices are 32-bit elements; how exact they have to be, the bound alone decides.
A program may use at most 64 MiB of HBM per device.

```python
import math
import jax
import jax.numpy as jnp
from jax import lax

D = 2048
QUERY_WIDTH = 1024
KEY_WIDTH = 512
RANK = 128
TOKENS = 8192
N_FS = 8


def draw_normed_input(key, part):
    first_key, second_key = jax.random.split(jax.random.fold_in(key, 17), 2)
    position = jnp.arange(D, dtype=jnp.float32) / D
    roughness = jnp.exp(jax.random.uniform(second_key, (D,), jnp.float32, -0.7, 0.7))
    entries = jax.random.normal(first_key, (TOKENS, D), jnp.float32)
    values = entries * 10.0 ** position * roughness
    return jnp.clip(values, -64.0, 64.0).astype(jnp.bfloat16)


def factor_draw(key, row_count, offset_seed):
    first_key, second_key = jax.random.split(jax.random.fold_in(key, offset_seed))
    entries = jax.random.normal(first_key, (row_count, RANK), jnp.float32)
    spread = jnp.exp(jax.random.uniform(second_key, (RANK,), jnp.float32, -1.15, 1.15))
    values = entries * spread / jnp.sqrt(jnp.float32(row_count))
    return jnp.clip(values, -1.0, 1.0).astype(jnp.bfloat16)


def draw_query_basis(key, part):
    return factor_draw(key, QUERY_WIDTH, 31)


def draw_key_basis(key, part):
    return factor_draw(key, KEY_WIDTH, 43)


def block_scale(rng, shape, pieces, least, top_value):
    def one(dim, shards_of):
        heights = jax.random.uniform(jax.random.fold_in(jax.random.fold_in(rng, 6), dim), (shards_of,), jnp.float32, least / len(pieces), top_value / len(pieces))
        return jnp.repeat(jnp.exp(heights), shape[dim] // shards_of).reshape((-1,) + (1,) * (len(shape) - dim - 1))

    loudness = one(*pieces[0])
    for cut in pieces[1:]:
        loudness = loudness * one(*cut)
    return loudness


def centred(rng, dims, scale, most, cuts=(), held_as=jnp.bfloat16):
    values = jax.random.normal(rng, dims, jnp.float32) * scale
    if len(cuts) > 0:
        values = block_scale(rng, dims, cuts, -0.22, 0.18) * values
    return jnp.clip(values, min=-most, max=most).astype(held_as)


def setup_inputs(seed: int = 0) -> dict:
    key_list = jax.random.split(jax.random.key(seed), 10)
    return {
        "normed_input": draw_normed_input(jax.random.fold_in(key_list[9], 71), 0),
        "query_cotangent": centred(key_list[1], (TOKENS, QUERY_WIDTH), 1.0, 6.0, ((0, 8), (1, 4))),
        "key_cotangent": centred(key_list[2], (TOKENS, KEY_WIDTH), 1.0, 6.0, ((0, 8), (1, 4))),
        "query_weight": centred(key_list[3], (D, QUERY_WIDTH), 1.0, 6.0, ((0, 8), (1, 4)), jnp.float32),
        "key_weight": centred(key_list[4], (D, KEY_WIDTH), 1.0, 6.0, ((0, 8), (1, 4)), jnp.float32),
        "query_basis": draw_query_basis(jax.random.fold_in(key_list[9], 71), 0),
        "key_basis": draw_key_basis(jax.random.fold_in(key_list[9], 71), 0),
        "moment_mean": centred(key_list[7], (2, D, RANK), 0.5, 3.0, ((1, 8),), jnp.float32),
        "moment_square": jnp.clip(jnp.exp(math.log(4.0) - 2.7725887 * jax.random.uniform(key_list[8], (2, D, RANK), jnp.float32) ** block_scale(key_list[8], (2, D, RANK), ((1, 8),), -0.2, 0.2)), 0.25, 4.0),
    }


BETA_MEAN = 0.75
BETA_SQUARE = 0.8
STEP_RATE = 0.25
EPSILON = 1e-06

def gradient_sum(inputs, cotangent):
    columns = cotangent.shape[1]
    input_blocks = inputs.reshape(N_FS, inputs.shape[0] // N_FS, inputs.shape[1])
    cotangent_blocks = cotangent.reshape(N_FS, cotangent.shape[0] // N_FS, columns)

    def accumulate(running_sum, operands):
        input_rows, cotangent_rows = operands
        product = lax.dot_general(input_rows.astype(jnp.float32), cotangent_rows.astype(jnp.float32), (((0,), (0,)), ((), ())), precision=lax.Precision.HIGHEST, preferred_element_type=jnp.float32)
        return (running_sum + product, None)
    initial = jnp.zeros((inputs.shape[1], columns), jnp.float32)
    running_sum, unused = lax.scan(accumulate, initial, (input_blocks, cotangent_blocks))
    return running_sum

def reference(normed_input, query_cotangent, key_cotangent, query_weight, key_weight, query_basis, key_basis, moment_mean, moment_square):
    query_float = query_basis.astype(jnp.float32)
    key_float = key_basis.astype(jnp.float32)
    query_gradient = gradient_sum(normed_input, query_cotangent)
    key_gradient = gradient_sum(normed_input, key_cotangent)
    query_projected = jnp.dot(query_gradient, query_float, precision=lax.Precision.HIGHEST)
    key_projected = jnp.dot(key_gradient, key_float, precision=lax.Precision.HIGHEST)
    projected = jnp.stack([query_projected, key_projected])
    mean_square = jnp.sum(projected * projected) / (2.0 * projected.shape[1] * projected.shape[2])
    normalized = projected * lax.rsqrt(mean_square + EPSILON)
    mean_updated = BETA_MEAN * moment_mean + (1.0 - BETA_MEAN) * normalized
    square_updated = BETA_SQUARE * moment_square + (1.0 - BETA_SQUARE) * normalized * normalized
    direction = mean_updated / jnp.sqrt(square_updated)
    query_step = jnp.dot(direction[0], query_float.T, precision=lax.Precision.HIGHEST)
    key_step = jnp.dot(direction[1], key_float.T, precision=lax.Precision.HIGHEST)
    query_updated = query_weight - STEP_RATE * query_step
    key_updated = key_weight - STEP_RATE * key_step
    return (query_step, key_step, query_updated, key_updated, query_updated.astype(jnp.bfloat16), key_updated.astype(jnp.bfloat16), mean_updated, square_updated)
```

```python
import functools

import jax
import jax.numpy as jnp
from jax import lax
from jax.experimental import pallas as pl
from jax.experimental.pallas import tpu as pltpu
from jax.sharding import PartitionSpec as P

BETA_MEAN = 0.75
BETA_SQUARE = 0.8
STEP_RATE = 0.25
EPSILON = 1e-06
CHUNKS = 4
MESH = pl.DeviceIdType.MESH
NT = (((1,), (1,)), ((), ()))


def split(value):
    high = value.astype(jnp.bfloat16)
    low = (value - high.astype(jnp.float32)).astype(jnp.bfloat16)
    return high, low


def reduce_kernel(
    n_fs,
    n_tp,
    x_hbm,
    cq_hbm,
    ck_hbm,
    bq_ref,
    bk_ref,
    out_ref,
    total_ref,
    x_ref,
    cq_ref,
    ck_ref,
    ybuf,
    ycore,
    ysum,
    yrecv,
    pbuf,
    xrecv,
    qbuf,
    zrecv,
    gather,
    square,
    squares,
    load_sem,
    core_send,
    core_recv,
    y_send,
    y_recv,
    x_send,
    x_recv,
    z_send,
    z_recv,
    g_send,
    g_recv,
    s_send,
    s_recv,
):
    f = lax.axis_index("fs")
    t = lax.axis_index("tp")
    tp_outer, fs_outer = n_tp // 2, n_fs // 2
    y, core = t // 2, t % 2
    z, x = f // 2, f % 2
    chunks, depth = ybuf.shape[0], ybuf.shape[3]
    rows = pbuf.shape[-1]
    rank = bq_ref.shape[1]

    def peer(df, dt):
        return (lax.rem(f + df, n_fs), lax.rem(t + dt, n_tp))

    others = [(df, dt) for df in range(n_fs) for dt in range(n_tp) if df or dt]

    loads = [
        pltpu.make_async_copy(cq_hbm, cq_ref, load_sem.at[0]),
        pltpu.make_async_copy(ck_hbm, ck_ref, load_sem.at[1]),
        pltpu.make_async_copy(x_hbm, x_ref, load_sem.at[2]),
    ]
    for load in loads:
        load.start()
    barrier = pltpu.get_barrier_semaphore()
    for df, dt in others:
        pl.semaphore_signal(barrier, inc=1, device_id=peer(df, dt), device_id_type=MESH)

    per = chunks * depth
    for which, (basis, cot) in enumerate(((bq_ref, cq_ref), (bk_ref, ck_ref))):
        loads[which].wait()
        part = lax.dot_general(
            basis[...].T, cot[...], NT, preferred_element_type=jnp.float32
        )
        for start in range(0, rank, depth):
            owner, c = divmod(which * rank + start, per)
            ybuf[c // depth, owner % 2, owner // 2] = part[start : start + depth]

    pl.semaphore_wait(barrier, len(others))

    def remote(src, dst, send, recv, device):
        return pltpu.make_async_remote_copy(
            src_ref=src, dst_ref=dst, send_sem=send, recv_sem=recv,
            device_id=device, device_id_type=MESH,
        )

    started = []

    core_copies = []
    for c in range(chunks):
        copy = remote(
            ybuf.at[c, 1 - core], ycore.at[c], core_send.at[c], core_recv.at[c],
            (f, y * 2 + 1 - core),
        )
        copy.start()
        core_copies.append(copy)
    started += core_copies

    y_copies = {}
    x_copies = {}
    z_copies = {}
    g_copies = {}

    def stage_core(c):
        core_copies[c].wait_recv()
        for o in range(tp_outer):
            ysum[c, o] = ybuf[c, core, o] + ycore[c, o]
        for d in range(1, tp_outer):
            to = lax.rem(y + d, tp_outer)
            copy = remote(
                ysum.at[c, to], yrecv.at[c, d - 1],
                y_send.at[c, d - 1], y_recv.at[c, d - 1], (f, to * 2 + core),
            )
            copy.start()
            y_copies[c, d] = copy
            started.append(copy)

    def stage_y(c):
        value = ysum[c, y]
        for d in range(1, tp_outer):
            y_copies[c, d].wait_recv()
            value = value + yrecv[c, d - 1]
        both = jnp.concatenate(split(value), axis=0)
        if c == 0:
            loads[2].wait()
        for o in range(fs_outer):
            wide = jnp.dot(
                both, x_ref[:, o * 2 * rows : (o + 1) * 2 * rows],
                preferred_element_type=jnp.float32,
            )
            wide = wide[:depth] + wide[depth:]
            pbuf[c, 0, o] = wide[:, :rows]
            pbuf[c, 1, o] = wide[:, rows:]
        copy = remote(
            pbuf.at[c, 1 - x], xrecv.at[c], x_send.at[c], x_recv.at[c],
            (z * 2 + 1 - x, t),
        )
        copy.start()
        x_copies[c] = copy
        started.append(copy)

    def stage_x(c):
        x_copies[c].wait_recv()
        for o in range(fs_outer):
            qbuf[c, o] = pbuf[c, x, o] + xrecv[c, o]
        for d in range(1, fs_outer):
            to = lax.rem(z + d, fs_outer)
            copy = remote(
                qbuf.at[c, to], zrecv.at[c, d - 1],
                z_send.at[c, d - 1], z_recv.at[c, d - 1], (to * 2 + x, t),
            )
            copy.start()
            z_copies[c, d] = copy
            started.append(copy)

    def stage_z(c):
        value = qbuf[c, z]
        for d in range(1, fs_outer):
            z_copies[c, d].wait_recv()
            value = value + zrecv[c, d - 1]
        gather[t, c] = value
        for d in range(1, n_tp):
            copy = remote(
                gather.at[t, c], gather.at[t, c],
                g_send.at[c, d - 1], g_recv.at[c, d - 1], peer(0, d),
            )
            copy.start()
            g_copies[c, d] = copy
            started.append(copy)
        powers = value * value
        acc = None
        for i in range(0, depth, 8):
            for j in range(0, rows, 128):
                piece = powers[i : i + 8, j : j + 128]
                acc = piece if acc is None else acc + piece
        return acc

    for c in range(chunks):
        stage_core(c)
    acc = None
    for step in range(chunks + 2):
        if step < chunks:
            stage_y(step)
        if 0 <= step - 1 < chunks:
            stage_x(step - 1)
        if 0 <= step - 2 < chunks:
            piece = stage_z(step - 2)
            acc = piece if acc is None else acc + piece

    square[...] = acc
    s_copies = []
    for i, (df, dt) in enumerate(others):
        copy = remote(square, squares.at[i], s_send.at[i], s_recv.at[i], peer(df, dt))
        copy.start()
        s_copies.append(copy)
    started += s_copies
    for c in range(chunks):
        for d in range(1, n_tp):
            g_copies[c, d].wait_recv()
    for o in range(n_tp):
        for c in range(chunks):
            out_ref[(o * chunks + c) * depth : (o * chunks + c + 1) * depth, :] = gather[o, c]
    for copy in s_copies:
        copy.wait_recv()
    for i in range(len(others)):
        acc = acc + squares[i]
    total_ref[...] = acc
    for copy in started:
        copy.wait_send()


def update_kernel(
    entry_count,
    sums_ref,
    total_ref,
    qw_ref,
    kw_ref,
    bq_ref,
    bk_ref,
    mean_ref,
    sq_ref,
    qs_out,
    ks_out,
    qu_out,
    ku_out,
    qc_out,
    kc_out,
    mean_out,
    sq_out,
):
    rank = bq_ref.shape[1]
    scale = lax.rsqrt(jnp.sum(total_ref[...], keepdims=True) / entry_count + EPSILON)
    sets = (
        (bq_ref, qw_ref, qs_out, qu_out, qc_out),
        (bk_ref, kw_ref, ks_out, ku_out, kc_out),
    )
    for which, (basis, weight, step_out, new_out, copy_out) in enumerate(sets):
        normalized = sums_ref[which * rank : (which + 1) * rank, :].T * scale
        mean = BETA_MEAN * mean_ref[which] + (1.0 - BETA_MEAN) * normalized
        second = BETA_SQUARE * sq_ref[which] + (1.0 - BETA_SQUARE) * normalized * normalized
        mean_out[which] = mean
        sq_out[which] = second
        high, low = split(mean / jnp.sqrt(second))
        step = lax.dot_general(high, basis[...], NT, preferred_element_type=jnp.float32)
        step += lax.dot_general(low, basis[...], NT, preferred_element_type=jnp.float32)
        new = weight[...] - STEP_RATE * step
        step_out[...] = step
        new_out[...] = new
        copy_out[...] = new.astype(jnp.bfloat16)


def fast(n_fs, n_tp, x, cq, ck, qw, kw, bq, bk, mean, sq):
    tokens, width = x.shape
    rows = qw.shape[0]
    rank = bq.shape[1]
    depth = 2 * rank // n_tp // CHUNKS
    tp_outer, fs_outer = n_tp // 2, n_fs // 2
    f32 = jnp.float32
    k = CHUNKS
    dma = pltpu.SemaphoreType.DMA
    hbm = pl.BlockSpec(memory_space=pl.ANY)
    vmem = pl.BlockSpec(memory_space=pltpu.VMEM)
    sums, total = pl.pallas_call(
        functools.partial(reduce_kernel, n_fs, n_tp),
        out_shape=(
            jax.ShapeDtypeStruct((2 * rank, rows), f32),
            jax.ShapeDtypeStruct((8, 128), f32),
        ),
        in_specs=[hbm, hbm, hbm, vmem, vmem],
        out_specs=(vmem, vmem),
        scratch_shapes=[
            pltpu.VMEM(x.shape, x.dtype),
            pltpu.VMEM(cq.shape, cq.dtype),
            pltpu.VMEM(ck.shape, ck.dtype),
            pltpu.VMEM((k, 2, tp_outer, depth, tokens), f32),
            pltpu.VMEM((k, tp_outer, depth, tokens), f32),
            pltpu.VMEM((k, tp_outer, depth, tokens), f32),
            pltpu.VMEM((k, tp_outer - 1, depth, tokens), f32),
            pltpu.VMEM((k, 2, fs_outer, depth, rows), f32),
            pltpu.VMEM((k, fs_outer, depth, rows), f32),
            pltpu.VMEM((k, fs_outer, depth, rows), f32),
            pltpu.VMEM((k, fs_outer - 1, depth, rows), f32),
            pltpu.VMEM((n_tp, k, depth, rows), f32),
            pltpu.VMEM((8, 128), f32),
            pltpu.VMEM((n_fs * n_tp - 1, 8, 128), f32),
            dma((3,)),
            dma((k,)),
            dma((k,)),
            dma((k, tp_outer - 1)),
            dma((k, tp_outer - 1)),
            dma((k,)),
            dma((k,)),
            dma((k, fs_outer - 1)),
            dma((k, fs_outer - 1)),
            dma((k, n_tp - 1)),
            dma((k, n_tp - 1)),
            dma((n_fs * n_tp - 1,)),
            dma((n_fs * n_tp - 1,)),
        ],
        compiler_params=pltpu.CompilerParams(
            collective_id=0, has_side_effects=True, vmem_limit_bytes=24 * 2**20
        ),
        cost_estimate=pl.CostEstimate(
            flops=4 * tokens * width * 2 * rank, bytes_accessed=2**24, transcendentals=0
        ),
    )(x, cq, ck, bq, bk)
    shape = jax.ShapeDtypeStruct
    bf16 = jnp.bfloat16
    return pl.pallas_call(
        functools.partial(update_kernel, 2.0 * rows * n_fs * rank),
        out_shape=(
            shape(qw.shape, f32),
            shape(kw.shape, f32),
            shape(qw.shape, f32),
            shape(kw.shape, f32),
            shape(qw.shape, bf16),
            shape(kw.shape, bf16),
            shape(mean.shape, f32),
            shape(sq.shape, f32),
        ),
        compiler_params=pltpu.CompilerParams(vmem_limit_bytes=24 * 2**20),
    )(sums, total, qw, kw, bq, bk, mean, sq)


def plain(x, cq, ck, qw, kw, bq, bk, mean, sq):
    highest = lax.Precision.HIGHEST
    contract = (((0,), (0,)), ((), ()))
    f32 = jnp.float32
    bq, bk = bq.astype(f32), bk.astype(f32)
    rows, rank = qw.shape[0], bq.shape[1]
    parts = []
    for cot, basis in ((cq, bq), (ck, bk)):
        gradient = lax.dot_general(x, cot, contract, preferred_element_type=f32)
        parts.append(jnp.dot(gradient, basis, precision=lax.Precision.HIGH))
    summed = lax.psum_scatter(
        jnp.concatenate(parts, axis=1), "fs", scatter_dimension=0, tiled=True
    )
    projected = lax.psum(jnp.stack([summed[:, :rank], summed[:, rank:]]), "tp")
    total = lax.psum(jnp.sum(projected * projected), "fs")
    count = 2.0 * rows * lax.axis_size("fs") * rank
    normalized = projected * lax.rsqrt(total / count + EPSILON)
    mean = BETA_MEAN * mean + (1.0 - BETA_MEAN) * normalized
    sq = BETA_SQUARE * sq + (1.0 - BETA_SQUARE) * normalized * normalized
    direction = mean / jnp.sqrt(sq)
    query_step = lax.dot_general(direction[0], bq, NT, precision=highest)
    key_step = lax.dot_general(direction[1], bk, NT, precision=highest)
    query_new = qw - STEP_RATE * query_step
    key_new = kw - STEP_RATE * key_step
    return (
        query_step,
        key_step,
        query_new,
        key_new,
        query_new.astype(jnp.bfloat16),
        key_new.astype(jnp.bfloat16),
        mean,
        sq,
    )


def solution(mesh):
    n_fs, n_tp = mesh.shape["fs"], mesh.shape["tp"]

    def local(x, cq, ck, qw, kw, bq, bk, mean, sq):
        rows, rank = qw.shape[0], bq.shape[1]
        fits = (
            n_fs % 2 == 0
            and n_tp % 2 == 0
            and n_fs > 2
            and n_tp > 2
            and rows % 128 == 0
            and rank % (n_tp // 2 * CHUNKS * 8) == 0
        )
        if fits:
            return fast(n_fs, n_tp, x, cq, ck, qw, kw, bq, bk, mean, sq)
        return plain(x, cq, ck, qw, kw, bq, bk, mean, sq)

    in_specs = (
        P("fs", None),
        P("fs", "tp"),
        P("fs", "tp"),
        P("fs", "tp"),
        P("fs", "tp"),
        P("tp", None),
        P("tp", None),
        P(None, "fs", None),
        P(None, "fs", None),
    )
    out_specs = (
        P("fs", "tp"),
        P("fs", "tp"),
        P("fs", "tp"),
        P("fs", "tp"),
        P("fs", "tp"),
        P("fs", "tp"),
        P(None, "fs", None),
        P(None, "fs", None),
    )
    return jax.shard_map(local, mesh=mesh, in_specs=in_specs, out_specs=out_specs, check_vma=False)
```

```python
import functools

import jax
import jax.numpy as jnp
from jax import lax
from jax.experimental import pallas as pl
from jax.experimental.pallas import tpu as pltpu
from jax.sharding import PartitionSpec as P

BETA_MEAN = 0.75
BETA_SQUARE = 0.8
STEP_RATE = 0.25
EPSILON = 1e-06
CHUNKS = 2
MESH = pl.DeviceIdType.MESH
NT = (((1,), (1,)), ((), ()))


def split(value):
    high = value.astype(jnp.bfloat16)
    low = (value - high.astype(jnp.float32)).astype(jnp.bfloat16)
    return high, low


def reduce_kernel(
    n_fs,
    n_tp,
    x_hbm,
    cq_hbm,
    ck_hbm,
    bq_hbm,
    bk_hbm,
    out_ref,
    total_ref,
    x_ref,
    cq_ref,
    ck_ref,
    bq_ref,
    bk_ref,
    ybuf,
    ycore,
    ysum,
    yrecv,
    pbuf,
    xrecv,
    qbuf,
    zrecv,
    gather,
    square,
    squares,
    load_sem,
    core_send,
    core_recv,
    y_send,
    y_recv,
    x_send,
    x_recv,
    z_send,
    z_recv,
    g_send,
    g_recv,
    s_send,
    s_recv,
):
    f = lax.axis_index("fs")
    t = lax.axis_index("tp")
    tp_outer, fs_outer = n_tp // 2, n_fs // 2
    y, core = t // 2, t % 2
    z, x = f // 2, f % 2
    chunks, depth = ybuf.shape[0], ybuf.shape[3]
    rows = pbuf.shape[-1]
    rank = bq_ref.shape[1]

    def peer(df, dt):
        return (lax.rem(f + df, n_fs), lax.rem(t + dt, n_tp))

    others = [(df, dt) for df in range(n_fs) for dt in range(n_tp) if df or dt]

    pairs = (
        (bq_hbm, bq_ref),
        (cq_hbm, cq_ref),
        (bk_hbm, bk_ref),
        (ck_hbm, ck_ref),
        (x_hbm, x_ref),
    )
    loads = [
        pltpu.make_async_copy(src, dst, load_sem.at[i])
        for i, (src, dst) in enumerate(pairs)
    ]
    barrier = pltpu.get_barrier_semaphore()
    for df, dt in reversed(others):
        pl.semaphore_signal(barrier, inc=1, device_id=peer(df, dt), device_id_type=MESH)
    for load in loads:
        load.start()

    per = chunks * depth
    for which, (basis, cot) in enumerate(((bq_ref, cq_ref), (bk_ref, ck_ref))):
        loads[2 * which].wait()
        loads[2 * which + 1].wait()
        part = lax.dot_general(
            basis[...].T, cot[...], NT, preferred_element_type=jnp.float32
        )
        for start in range(0, rank, depth):
            owner, c = divmod(which * rank + start, per)
            ybuf[c // depth, owner % 2, owner // 2] = part[start : start + depth]

    pl.semaphore_wait(barrier, len(others))

    def remote(src, dst, send, recv, device):
        return pltpu.make_async_remote_copy(
            src_ref=src, dst_ref=dst, send_sem=send, recv_sem=recv,
            device_id=device, device_id_type=MESH,
        )

    started = []

    core_copies = []
    for c in range(chunks):
        copy = remote(
            ybuf.at[c, 1 - core], ycore.at[c], core_send.at[c], core_recv.at[c],
            (f, y * 2 + 1 - core),
        )
        copy.start()
        core_copies.append(copy)
    started += core_copies

    y_copies = {}
    x_copies = {}
    order = sorted(range(1, fs_outer), key=lambda j: abs(2 * j - fs_outer)) + [0]
    z_copies = {}
    g_copies = {}

    def stage_core(c):
        core_copies[c].wait_recv()
        for o in range(tp_outer):
            ysum[c, o] = ybuf[c, core, o] + ycore[c, o]
        for d in range(1, tp_outer):
            to = lax.rem(y + d, tp_outer)
            copy = remote(
                ysum.at[c, to], yrecv.at[c, d - 1],
                y_send.at[c, d - 1], y_recv.at[c, d - 1], (f, to * 2 + core),
            )
            copy.start()
            y_copies[c, d] = copy
            started.append(copy)

    def stage_y(c):
        value = ysum[c, y]
        for d in range(1, tp_outer):
            y_copies[c, d].wait_recv()
            value = value + yrecv[c, d - 1]
        both = jnp.concatenate(split(value), axis=0)
        if c == 0:
            loads[4].wait()
        for o in range(fs_outer):
            wide = jnp.dot(
                both, x_ref[:, o * 2 * rows : (o + 1) * 2 * rows],
                preferred_element_type=jnp.float32,
            )
            wide = wide[:depth] + wide[depth:]
            pbuf[c, 0, o] = wide[:, :rows]
            pbuf[c, 1, o] = wide[:, rows:]
        for j in order:
            copy = remote(
                pbuf.at[c, 1 - x, lax.rem(z + j, fs_outer)], xrecv.at[c, j],
                x_send.at[c, j], x_recv.at[c, j], (z * 2 + 1 - x, t),
            )
            copy.start()
            x_copies[c, j] = copy
            started.append(copy)

    def stage_x(c):
        for j in order:
            to = lax.rem(z + j, fs_outer)
            x_copies[c, j].wait_recv()
            qbuf[c, j] = pbuf[c, x, to] + xrecv[c, j]
            if j == 0:
                continue
            copy = remote(
                qbuf.at[c, j], zrecv.at[c, j - 1],
                z_send.at[c, j - 1], z_recv.at[c, j - 1], (to * 2 + x, t),
            )
            copy.start()
            z_copies[c, j] = copy
            started.append(copy)

    def stage_z(c):
        value = qbuf[c, 0]
        for d in range(1, fs_outer):
            z_copies[c, d].wait_recv()
            value = value + zrecv[c, d - 1]
        gather[t, c] = value
        for d in range(1, n_tp):
            copy = remote(
                gather.at[t, c], gather.at[t, c],
                g_send.at[c, d - 1], g_recv.at[c, d - 1], peer(0, d),
            )
            copy.start()
            g_copies[c, d] = copy
            started.append(copy)
        powers = value * value
        acc = None
        for i in range(0, depth, 8):
            for j in range(0, rows, 128):
                piece = powers[i : i + 8, j : j + 128]
                acc = piece if acc is None else acc + piece
        return acc

    for c in range(chunks):
        stage_core(c)
    acc = None
    for step in range(chunks + 2):
        if step < chunks:
            stage_y(step)
        if 0 <= step - 1 < chunks:
            stage_x(step - 1)
        if 0 <= step - 2 < chunks:
            piece = stage_z(step - 2)
            acc = piece if acc is None else acc + piece

    acc = jnp.sum(acc, axis=0, keepdims=True)
    square[...] = acc
    s_copies = []
    for i, (df, dt) in enumerate(others):
        copy = remote(square, squares.at[i], s_send.at[i], s_recv.at[i], peer(df, dt))
        copy.start()
        s_copies.append(copy)
    started += s_copies
    for c in range(chunks):
        for d in range(1, n_tp):
            g_copies[c, d].wait_recv()
    for o in range(n_tp):
        for c in range(chunks):
            out_ref[(o * chunks + c) * depth : (o * chunks + c + 1) * depth, :] = gather[o, c]
    for copy in s_copies:
        copy.wait_recv()
    for i in range(len(others)):
        acc = acc + squares[i]
    total_ref[...] = acc
    for copy in started:
        copy.wait_send()


def update_kernel(
    entry_count,
    sums_ref,
    total_ref,
    qw_ref,
    kw_ref,
    bq_ref,
    bk_ref,
    mean_ref,
    sq_ref,
    qs_out,
    ks_out,
    qu_out,
    ku_out,
    qc_out,
    kc_out,
    mean_out,
    sq_out,
):
    rank = bq_ref.shape[1]
    scale = lax.rsqrt(jnp.sum(total_ref[...], keepdims=True) / entry_count + EPSILON)
    sets = (
        (bq_ref, qw_ref, qs_out, qu_out, qc_out),
        (bk_ref, kw_ref, ks_out, ku_out, kc_out),
    )
    for which, (basis, weight, step_out, new_out, copy_out) in enumerate(sets):
        normalized = sums_ref[which * rank : (which + 1) * rank, :].T * scale
        mean = BETA_MEAN * mean_ref[which] + (1.0 - BETA_MEAN) * normalized
        second = BETA_SQUARE * sq_ref[which] + (1.0 - BETA_SQUARE) * normalized * normalized
        mean_out[which] = mean
        sq_out[which] = second
        high, low = split(mean / jnp.sqrt(second))
        step = lax.dot_general(high, basis[...], NT, preferred_element_type=jnp.float32)
        step += lax.dot_general(low, basis[...], NT, preferred_element_type=jnp.float32)
        new = weight[...] - STEP_RATE * step
        step_out[...] = step
        new_out[...] = new
        copy_out[...] = new.astype(jnp.bfloat16)


def fast(n_fs, n_tp, x, cq, ck, qw, kw, bq, bk, mean, sq):
    tokens, width = x.shape
    rows = qw.shape[0]
    rank = bq.shape[1]
    depth = 2 * rank // n_tp // CHUNKS
    tp_outer, fs_outer = n_tp // 2, n_fs // 2
    f32 = jnp.float32
    k = CHUNKS
    dma = pltpu.SemaphoreType.DMA
    hbm = pl.BlockSpec(memory_space=pl.ANY)
    vmem = pl.BlockSpec(memory_space=pltpu.VMEM)
    sums, total = pl.pallas_call(
        functools.partial(reduce_kernel, n_fs, n_tp),
        out_shape=(
            jax.ShapeDtypeStruct((2 * rank, rows), f32),
            jax.ShapeDtypeStruct((1, 128), f32),
        ),
        in_specs=[hbm] * 5,
        out_specs=(vmem, vmem),
        scratch_shapes=[
            pltpu.VMEM(x.shape, x.dtype),
            pltpu.VMEM(cq.shape, cq.dtype),
            pltpu.VMEM(ck.shape, ck.dtype),
            pltpu.VMEM(bq.shape, bq.dtype),
            pltpu.VMEM(bk.shape, bk.dtype),
            pltpu.VMEM((k, 2, tp_outer, depth, tokens), f32),
            pltpu.VMEM((k, tp_outer, depth, tokens), f32),
            pltpu.VMEM((k, tp_outer, depth, tokens), f32),
            pltpu.VMEM((k, tp_outer - 1, depth, tokens), f32),
            pltpu.VMEM((k, 2, fs_outer, depth, rows), f32),
            pltpu.VMEM((k, fs_outer, depth, rows), f32),
            pltpu.VMEM((k, fs_outer, depth, rows), f32),
            pltpu.VMEM((k, fs_outer - 1, depth, rows), f32),
            pltpu.VMEM((n_tp, k, depth, rows), f32),
            pltpu.VMEM((1, 128), f32),
            pltpu.VMEM((n_fs * n_tp - 1, 1, 128), f32),
            dma((5,)),
            dma((k,)),
            dma((k,)),
            dma((k, tp_outer - 1)),
            dma((k, tp_outer - 1)),
            dma((k, fs_outer)),
            dma((k, fs_outer)),
            dma((k, fs_outer - 1)),
            dma((k, fs_outer - 1)),
            dma((k, n_tp - 1)),
            dma((k, n_tp - 1)),
            dma((n_fs * n_tp - 1,)),
            dma((n_fs * n_tp - 1,)),
        ],
        compiler_params=pltpu.CompilerParams(
            collective_id=0, has_side_effects=True, vmem_limit_bytes=60 * 2**20
        ),
        cost_estimate=pl.CostEstimate(
            flops=4 * tokens * width * 2 * rank, bytes_accessed=2**24, transcendentals=0
        ),
    )(x, cq, ck, bq, bk)
    shape = jax.ShapeDtypeStruct
    bf16 = jnp.bfloat16
    return pl.pallas_call(
        functools.partial(update_kernel, 2.0 * rows * n_fs * rank),
        out_shape=(
            shape(qw.shape, f32),
            shape(kw.shape, f32),
            shape(qw.shape, f32),
            shape(kw.shape, f32),
            shape(qw.shape, bf16),
            shape(kw.shape, bf16),
            shape(mean.shape, f32),
            shape(sq.shape, f32),
        ),
        compiler_params=pltpu.CompilerParams(vmem_limit_bytes=24 * 2**20),
    )(sums, total, qw, kw, bq, bk, mean, sq)


def plain(x, cq, ck, qw, kw, bq, bk, mean, sq):
    highest = lax.Precision.HIGHEST
    contract = (((0,), (0,)), ((), ()))
    f32 = jnp.float32
    bq, bk = bq.astype(f32), bk.astype(f32)
    rows, rank = qw.shape[0], bq.shape[1]
    parts = []
    for cot, basis in ((cq, bq), (ck, bk)):
        gradient = lax.dot_general(x, cot, contract, preferred_element_type=f32)
        parts.append(jnp.dot(gradient, basis, precision=lax.Precision.HIGH))
    summed = lax.psum_scatter(
        jnp.concatenate(parts, axis=1), "fs", scatter_dimension=0, tiled=True
    )
    projected = lax.psum(jnp.stack([summed[:, :rank], summed[:, rank:]]), "tp")
    total = lax.psum(jnp.sum(projected * projected), "fs")
    count = 2.0 * rows * lax.axis_size("fs") * rank
    normalized = projected * lax.rsqrt(total / count + EPSILON)
    mean = BETA_MEAN * mean + (1.0 - BETA_MEAN) * normalized
    sq = BETA_SQUARE * sq + (1.0 - BETA_SQUARE) * normalized * normalized
    direction = mean / jnp.sqrt(sq)
    query_step = lax.dot_general(direction[0], bq, NT, precision=highest)
    key_step = lax.dot_general(direction[1], bk, NT, precision=highest)
    query_new = qw - STEP_RATE * query_step
    key_new = kw - STEP_RATE * key_step
    return (
        query_step,
        key_step,
        query_new,
        key_new,
        query_new.astype(jnp.bfloat16),
        key_new.astype(jnp.bfloat16),
        mean,
        sq,
    )


def solution(mesh):
    n_fs, n_tp = mesh.shape["fs"], mesh.shape["tp"]

    def local(x, cq, ck, qw, kw, bq, bk, mean, sq):
        rows, rank = qw.shape[0], bq.shape[1]
        fits = (
            n_fs % 2 == 0
            and n_tp % 2 == 0
            and n_fs > 2
            and n_tp > 2
            and rows % 128 == 0
            and rank % (n_tp // 2 * CHUNKS * 8) == 0
        )
        if fits:
            return fast(n_fs, n_tp, x, cq, ck, qw, kw, bq, bk, mean, sq)
        return plain(x, cq, ck, qw, kw, bq, bk, mean, sq)

    in_specs = (
        P("fs", None),
        P("fs", "tp"),
        P("fs", "tp"),
        P("fs", "tp"),
        P("fs", "tp"),
        P("tp", None),
        P("tp", None),
        P(None, "fs", None),
        P(None, "fs", None),
    )
    out_specs = (
        P("fs", "tp"),
        P("fs", "tp"),
        P("fs", "tp"),
        P("fs", "tp"),
        P("fs", "tp"),
        P("fs", "tp"),
        P(None, "fs", None),
        P(None, "fs", None),
    )
    return jax.shard_map(local, mesh=mesh, in_specs=in_specs, out_specs=out_specs, check_vma=False)
```

```python
import functools

import jax
import jax.numpy as jnp
from jax import lax
from jax.experimental import pallas as pl
from jax.experimental.pallas import tpu as pltpu
from jax.sharding import PartitionSpec as P

BETA_MEAN = 0.75
BETA_SQUARE = 0.8
STEP_RATE = 0.25
EPSILON = 1e-06
CHUNKS = 2
MESH = pl.DeviceIdType.MESH
NT = (((1,), (1,)), ((), ()))


def split(value):
    high = value.astype(jnp.bfloat16)
    low = (value - high.astype(jnp.float32)).astype(jnp.bfloat16)
    return high, low


def reduce_kernel(
    n_fs,
    n_tp,
    x_hbm,
    cq_hbm,
    ck_hbm,
    bq_hbm,
    bk_hbm,
    out_ref,
    total_ref,
    x_ref,
    cq_ref,
    ck_ref,
    bq_ref,
    bk_ref,
    ybuf,
    ycore,
    ysum,
    yrecv,
    pbuf,
    xrecv,
    qbuf,
    zrecv,
    gather,
    square,
    squares,
    load_sem,
    core_send,
    core_recv,
    y_send,
    y_recv,
    x_send,
    x_recv,
    z_send,
    z_recv,
    g_send,
    g_recv,
    s_send,
    s_recv,
):
    f = lax.axis_index("fs")
    t = lax.axis_index("tp")
    tp_outer, fs_outer = n_tp // 2, n_fs // 2
    y, core = t // 2, t % 2
    z, x = f // 2, f % 2
    chunks, depth = ybuf.shape[0], ybuf.shape[3]
    rows = pbuf.shape[-1]
    rank = bq_ref.shape[1]

    def peer(df, dt):
        return (lax.rem(f + df, n_fs), lax.rem(t + dt, n_tp))

    others = [(df, dt) for df in range(n_fs) for dt in range(n_tp) if df or dt]

    pairs = (
        (bq_hbm, bq_ref),
        (cq_hbm, cq_ref),
        (bk_hbm, bk_ref),
        (ck_hbm, ck_ref),
        (x_hbm, x_ref),
    )
    loads = [
        pltpu.make_async_copy(src, dst, load_sem.at[i])
        for i, (src, dst) in enumerate(pairs)
    ]
    barrier = pltpu.get_barrier_semaphore()
    for df, dt in reversed(others):
        pl.semaphore_signal(barrier, inc=1, device_id=peer(df, dt), device_id_type=MESH)
    for load in loads:
        load.start()

    per = chunks * depth
    for which, (basis, cot) in enumerate(((bq_ref, cq_ref), (bk_ref, ck_ref))):
        loads[2 * which].wait()
        loads[2 * which + 1].wait()
        part = lax.dot_general(
            basis[...].T, cot[...], NT, preferred_element_type=jnp.float32
        )
        for start in range(0, rank, depth):
            owner, c = divmod(which * rank + start, per)
            ybuf[c // depth, owner % 2, owner // 2] = part[start : start + depth]

    pl.semaphore_wait(barrier, len(others))

    def remote(src, dst, send, recv, device):
        return pltpu.make_async_remote_copy(
            src_ref=src, dst_ref=dst, send_sem=send, recv_sem=recv,
            device_id=device, device_id_type=MESH,
        )

    started = []

    core_copies = []
    for c in range(chunks):
        copy = remote(
            ybuf.at[c, 1 - core], ycore.at[c], core_send.at[c], core_recv.at[c],
            (f, y * 2 + 1 - core),
        )
        copy.start()
        core_copies.append(copy)
    started += core_copies

    y_copies = {}
    x_copies = {}
    order = sorted(range(1, fs_outer), key=lambda j: abs(2 * j - fs_outer)) + [0]
    z_copies = {}
    g_copies = {}

    def stage_core(c):
        core_copies[c].wait_recv()
        for o in range(tp_outer):
            ysum[c, o] = ybuf[c, core, o] + ycore[c, o]
        for d in range(1, tp_outer):
            to = lax.rem(y + d, tp_outer)
            copy = remote(
                ysum.at[c, to], yrecv.at[c, d - 1],
                y_send.at[c, d - 1], y_recv.at[c, d - 1], (f, to * 2 + core),
            )
            copy.start()
            y_copies[c, d] = copy
            started.append(copy)

    def stage_y(c):
        value = ysum[c, y]
        for d in range(1, tp_outer):
            y_copies[c, d].wait_recv()
            value = value + yrecv[c, d - 1]
        both = jnp.concatenate(split(value), axis=0)
        if c == 0:
            loads[4].wait()
        for o in range(fs_outer):
            wide = jnp.dot(
                both, x_ref[:, o * 2 * rows : (o + 1) * 2 * rows],
                preferred_element_type=jnp.float32,
            )
            wide = wide[:depth] + wide[depth:]
            pbuf[c, 0, o] = wide[:, :rows]
            pbuf[c, 1, o] = wide[:, rows:]
        for j in order:
            copy = remote(
                pbuf.at[c, 1 - x, lax.rem(z + j, fs_outer)], xrecv.at[c, j],
                x_send.at[c, j], x_recv.at[c, j], (z * 2 + 1 - x, t),
            )
            copy.start()
            x_copies[c, j] = copy
            started.append(copy)

    def stage_x(c):
        for j in order:
            to = lax.rem(z + j, fs_outer)
            x_copies[c, j].wait_recv()
            qbuf[c, j] = pbuf[c, x, to] + xrecv[c, j]
            if j == 0:
                continue
            copy = remote(
                qbuf.at[c, j], zrecv.at[c, j - 1],
                z_send.at[c, j - 1], z_recv.at[c, j - 1], (to * 2 + x, t),
            )
            copy.start()
            z_copies[c, j] = copy
            started.append(copy)

    def stage_z(c):
        value = qbuf[c, 0]
        for d in range(1, fs_outer):
            z_copies[c, d].wait_recv()
            value = value + zrecv[c, d - 1]
        gather[t, c] = value
        for d in range(1, n_tp):
            copy = remote(
                gather.at[t, c], gather.at[t, c],
                g_send.at[c, d - 1], g_recv.at[c, d - 1], peer(0, d),
            )
            copy.start()
            g_copies[c, d] = copy
            started.append(copy)
        powers = value * value
        acc = None
        for i in range(0, depth, 8):
            for j in range(0, rows, 128):
                piece = powers[i : i + 8, j : j + 128]
                acc = piece if acc is None else acc + piece
        return acc

    for c in range(chunks):
        stage_core(c)
    acc = None
    for step in range(chunks + 2):
        if step < chunks:
            stage_y(step)
        if 0 <= step - 1 < chunks:
            stage_x(step - 1)
        if 0 <= step - 2 < chunks:
            piece = stage_z(step - 2)
            acc = piece if acc is None else acc + piece

    acc = jnp.sum(acc, axis=0, keepdims=True)
    square[...] = acc
    s_copies = []
    for i, (df, dt) in enumerate(others):
        copy = remote(square, squares.at[i], s_send.at[i], s_recv.at[i], peer(df, dt))
        copy.start()
        s_copies.append(copy)
    started += s_copies
    for c in range(chunks):
        for d in range(1, n_tp):
            g_copies[c, d].wait_recv()
    for o in range(n_tp):
        for c in range(chunks):
            out_ref[(o * chunks + c) * depth : (o * chunks + c + 1) * depth, :] = gather[o, c]
    for copy in s_copies:
        copy.wait_recv()
    for i in range(len(others)):
        acc = acc + squares[i]
    total_ref[...] = acc
    for copy in started:
        copy.wait_send()


def update_kernel(
    entry_count,
    sums_ref,
    total_ref,
    qw_ref,
    kw_ref,
    bq_ref,
    bk_ref,
    mean_ref,
    sq_ref,
    qs_out,
    ks_out,
    qu_out,
    ku_out,
    qc_out,
    kc_out,
    mean_out,
    sq_out,
):
    rank = bq_ref.shape[1]
    scale = lax.rsqrt(jnp.sum(total_ref[...], keepdims=True) / entry_count + EPSILON)
    sets = (
        (bq_ref, qw_ref, qs_out, qu_out, qc_out),
        (bk_ref, kw_ref, ks_out, ku_out, kc_out),
    )
    for which, (basis, weight, step_out, new_out, copy_out) in enumerate(sets):
        normalized = sums_ref[which * rank : (which + 1) * rank, :].T * scale
        mean = BETA_MEAN * mean_ref[which] + (1.0 - BETA_MEAN) * normalized
        second = BETA_SQUARE * sq_ref[which] + (1.0 - BETA_SQUARE) * normalized * normalized
        mean_out[which] = mean
        sq_out[which] = second
        high, low = split(mean / jnp.sqrt(second))
        step = lax.dot_general(high, basis[...], NT, preferred_element_type=jnp.float32)
        step += lax.dot_general(low, basis[...], NT, preferred_element_type=jnp.float32)
        new = weight[...] - STEP_RATE * step
        step_out[...] = step
        new_out[...] = new
        copy_out[...] = new.astype(jnp.bfloat16)


def fast(n_fs, n_tp, x, cq, ck, qw, kw, bq, bk, mean, sq):
    tokens, width = x.shape
    rows = qw.shape[0]
    rank = bq.shape[1]
    depth = 2 * rank // n_tp // CHUNKS
    tp_outer, fs_outer = n_tp // 2, n_fs // 2
    f32 = jnp.float32
    k = CHUNKS
    dma = pltpu.SemaphoreType.DMA
    hbm = pl.BlockSpec(memory_space=pl.ANY)
    vmem = pl.BlockSpec(memory_space=pltpu.VMEM)
    sums, total = pl.pallas_call(
        functools.partial(reduce_kernel, n_fs, n_tp),
        out_shape=(
            pltpu.VMEM((2 * rank, rows), f32),
            pltpu.VMEM((1, 128), f32),
        ),
        in_specs=[hbm] * 5,
        out_specs=(vmem, vmem),
        scratch_shapes=[
            pltpu.VMEM(x.shape, x.dtype),
            pltpu.VMEM(cq.shape, cq.dtype),
            pltpu.VMEM(ck.shape, ck.dtype),
            pltpu.VMEM(bq.shape, bq.dtype),
            pltpu.VMEM(bk.shape, bk.dtype),
            pltpu.VMEM((k, 2, tp_outer, depth, tokens), f32),
            pltpu.VMEM((k, tp_outer, depth, tokens), f32),
            pltpu.VMEM((k, tp_outer, depth, tokens), f32),
            pltpu.VMEM((k, tp_outer - 1, depth, tokens), f32),
            pltpu.VMEM((k, 2, fs_outer, depth, rows), f32),
            pltpu.VMEM((k, fs_outer, depth, rows), f32),
            pltpu.VMEM((k, fs_outer, depth, rows), f32),
            pltpu.VMEM((k, fs_outer - 1, depth, rows), f32),
            pltpu.VMEM((n_tp, k, depth, rows), f32),
            pltpu.VMEM((1, 128), f32),
            pltpu.VMEM((n_fs * n_tp - 1, 1, 128), f32),
            dma((5,)),
            dma((k,)),
            dma((k,)),
            dma((k, tp_outer - 1)),
            dma((k, tp_outer - 1)),
            dma((k, fs_outer)),
            dma((k, fs_outer)),
            dma((k, fs_outer - 1)),
            dma((k, fs_outer - 1)),
            dma((k, n_tp - 1)),
            dma((k, n_tp - 1)),
            dma((n_fs * n_tp - 1,)),
            dma((n_fs * n_tp - 1,)),
        ],
        compiler_params=pltpu.CompilerParams(
            collective_id=0, has_side_effects=True, vmem_limit_bytes=60 * 2**20
        ),
        cost_estimate=pl.CostEstimate(
            flops=4 * tokens * width * 2 * rank, bytes_accessed=2**24, transcendentals=0
        ),
    )(x, cq, ck, bq, bk)
    shape = jax.ShapeDtypeStruct
    bf16 = jnp.bfloat16
    return pl.pallas_call(
        functools.partial(update_kernel, 2.0 * rows * n_fs * rank),
        out_shape=(
            shape(qw.shape, f32),
            shape(kw.shape, f32),
            shape(qw.shape, f32),
            shape(kw.shape, f32),
            shape(qw.shape, bf16),
            shape(kw.shape, bf16),
            shape(mean.shape, f32),
            shape(sq.shape, f32),
        ),
        compiler_params=pltpu.CompilerParams(vmem_limit_bytes=24 * 2**20),
    )(sums, total, qw, kw, bq, bk, mean, sq)


def plain(x, cq, ck, qw, kw, bq, bk, mean, sq):
    highest = lax.Precision.HIGHEST
    contract = (((0,), (0,)), ((), ()))
    f32 = jnp.float32
    bq, bk = bq.astype(f32), bk.astype(f32)
    rows, rank = qw.shape[0], bq.shape[1]
    parts = []
    for cot, basis in ((cq, bq), (ck, bk)):
        gradient = lax.dot_general(x, cot, contract, preferred_element_type=f32)
        parts.append(jnp.dot(gradient, basis, precision=lax.Precision.HIGH))
    summed = lax.psum_scatter(
        jnp.concatenate(parts, axis=1), "fs", scatter_dimension=0, tiled=True
    )
    projected = lax.psum(jnp.stack([summed[:, :rank], summed[:, rank:]]), "tp")
    total = lax.psum(jnp.sum(projected * projected), "fs")
    count = 2.0 * rows * lax.axis_size("fs") * rank
    normalized = projected * lax.rsqrt(total / count + EPSILON)
    mean = BETA_MEAN * mean + (1.0 - BETA_MEAN) * normalized
    sq = BETA_SQUARE * sq + (1.0 - BETA_SQUARE) * normalized * normalized
    direction = mean / jnp.sqrt(sq)
    query_step = lax.dot_general(direction[0], bq, NT, precision=highest)
    key_step = lax.dot_general(direction[1], bk, NT, precision=highest)
    query_new = qw - STEP_RATE * query_step
    key_new = kw - STEP_RATE * key_step
    return (
        query_step,
        key_step,
        query_new,
        key_new,
        query_new.astype(jnp.bfloat16),
        key_new.astype(jnp.bfloat16),
        mean,
        sq,
    )


def solution(mesh):
    n_fs, n_tp = mesh.shape["fs"], mesh.shape["tp"]

    def local(x, cq, ck, qw, kw, bq, bk, mean, sq):
        rows, rank = qw.shape[0], bq.shape[1]
        fits = (
            n_fs % 2 == 0
            and n_tp % 2 == 0
            and n_fs > 2
            and n_tp > 2
            and rows % 128 == 0
            and rank % (n_tp // 2 * CHUNKS * 8) == 0
        )
        if fits:
            return fast(n_fs, n_tp, x, cq, ck, qw, kw, bq, bk, mean, sq)
        return plain(x, cq, ck, qw, kw, bq, bk, mean, sq)

    in_specs = (
        P("fs", None),
        P("fs", "tp"),
        P("fs", "tp"),
        P("fs", "tp"),
        P("fs", "tp"),
        P("tp", None),
        P("tp", None),
        P(None, "fs", None),
        P(None, "fs", None),
    )
    out_specs = (
        P("fs", "tp"),
        P("fs", "tp"),
        P("fs", "tp"),
        P("fs", "tp"),
        P("fs", "tp"),
        P("fs", "tp"),
        P(None, "fs", None),
        P(None, "fs", None),
    )
    return jax.shard_map(local, mesh=mesh, in_specs=in_specs, out_specs=out_specs, check_vma=False)
```
